32 devices in a mesh: ep: 4 (over y, x), tp: 8 (over z, core).
Axes of the slice: x: 2, y: 2, z: 4, core: 2. Of those that a mesh axis runs over, the one named last changes fastest.
Arguments:
- tokens: bfloat16 [256, 4096], P('ep'), may hold values from -6 to 6
- norm_gain: float32 [4096], replicated, may hold values from 0.1 to 1.9
- ffn_gain: float32 [4096], replicated, may hold values from 0.1 to 1.9
- w_in: bfloat16 [4096, 2048], P(None, 'tp'), may hold values from -0.09375 to 0.09375
- decay_rate: float32 [8192], P('tp'), may hold values from 0.02 to 2
- frequency: float32 [8192], P('tp'), may hold values from -3.140625 to 3.140625
- log_step: float32 [128], P('tp'), may hold values from -2.3 to 0
- input_real: float32 [16, 8192], P(None, 'tp'), may hold values from -1 to 1
- input_imag: float32 [16, 8192], P(None, 'tp'), may hold values from -1 to 1
- readout_real: float32 [16, 8192], P(None, 'tp'), may hold values from -0.5 to 0.5
- readout_imag: float32 [16, 8192], P(None, 'tp'), may hold values from -0.5 to 0.5
- skip_gain: float32 [2048], P('tp'), may hold values from -4 to 4
- state_real: float32 [256, 8192], P('ep', 'tp'), may hold values from -6 to 6
- state_imag: float32 [256, 8192], P('ep', 'tp'), may hold values from -6 to 6
- w_out: bfloat16 [2048, 4096], P('tp'), may hold values from -0.125 to 0.125
- shared_gate: bfloat16 [4096, 1024], P(None, 'tp'), may hold values from -0.09375 to 0.09375
- shared_up: bfloat16 [4096, 1024], P(None, 'tp'), may hold values from -0.09375 to 0.09375
- shared_down: bfloat16 [1024, 4096], P('tp'), may hold values from -0.1875 to 0.1875
- expert_gate: bfloat16 [16, 4096, 1024], P('ep', 'tp'), may hold values from -0.09375 to 0.09375
- expert_up: bfloat16 [16, 4096, 1024], P('ep', 'tp'), may hold values from -0.09375 to 0.09375
- expert_down: bfloat16 [16, 1024, 4096], P('ep', None, 'tp'), may hold values from -0.1875 to 0.1875
- routing: int32 [256, 4], P('ep'), may hold values from 0 to 15, all different within a row; in each aligned block of 64 rows (0 to 63, 64 to 127, ...) at most 32 rows name the same one
- route_weight: float32 [256, 4], P('ep'), may hold values from 0.1 to 1
Outputs:
- mixed: bfloat16 [256, 4096], P('ep', 'tp')
- new_state_real: float32 [256, 8192], P('ep', 'tp')
- new_state_imag: float32 [256, 8192], P('ep', 'tp')
The draws below stay inside these ranges and needn't reach their ends.
Inputs may be any that keep to these rules, and one draw needn't show every extreme that they name: `routing`: each row names 4 different experts. In the rows of one index of ep (aligned blocks of 64 rows) no expert is named more than 32 times, and in every draw some expert is named exactly 32 times in some block.
All inputs are finite; a program needn't handle non-finite values.
Results may differ from the reference program's by a relative error of at most 0.02.
Values may be sent and summed in bfloat16 or wider, within the bound.
No kernel may reach another device: no remote copies, remote signals or barrier semaphores. Data moves between devices by JAX's collectives and lax.ppermute only.
A program may use at most 64 MiB of HBM per device.

```python
import math
import jax
import jax.numpy as jnp
import numpy as np
from jax import lax

D = 4096
GROUPS = 128
CHAN = 16
STATE = 64
FE = 1024
FS = 1024
TOP_K = 4
SEQ_DEV = 64
SEQS = 256
EXPERTS = 16
CAP = 32


def steps_of(rng, dims, pieces, low, high):
    loudness, own = 1.0, jax.random.fold_in(rng, 6)
    for axis_at, shards_of in pieces:
        heights = jnp.exp(jax.random.uniform(jax.random.fold_in(own, axis_at), (shards_of,), jnp.float32, low / len(pieces), high / len(pieces)))
        loudness = loudness * jnp.repeat(heights, dims[axis_at] // shards_of).reshape([-1 if axis == axis_at else 1 for axis in range(len(dims))])
    return loudness


def routed_block(key, own, number, rows, amount, top, most, skew):
    sequence = jax.random.permutation(key, amount)
    heavy_load, usual = load_shares(amount, rows * top, most, skew, True), load_shares(amount, rows * top, most, skew, False)
    places = jnp.arange(amount)

    def named(tallies, rotation):
        used = int((tallies > 0).sum())
        fixed = max(1, used // 4)
        shifted = fixed + (places - fixed + rotation * (used - fixed)) % max(1, amount - fixed)
        return jnp.zeros((amount,), jnp.int32).at[sequence[jnp.where(places < fixed, places, shifted)]].set(jnp.asarray(tallies, jnp.int32))

    tallies = jnp.where(number % 4 == 0, named(heavy_load, number // 4), named(usual, number - number // 4 - 1))
    mixed = jax.random.permutation(jax.random.fold_in(own, 3), amount)
    source_of, taker = mixed[0:amount // 2 * 2:2], mixed[1:amount // 2 * 2:2]
    margin = jnp.minimum(tallies[source_of] - 1, most - tallies[taker]) // 2
    margin = jnp.where((source_of == sequence[0]) | (taker == sequence[0]) | (tallies[taker] == 0), 0, jnp.maximum(margin, 0))
    shifted = jax.random.randint(jax.random.fold_in(own, 4), (amount // 2,), 0, 1 << 20) % (margin + 1)
    tallies = tallies.at[source_of].add(-shifted).at[taker].add(shifted)
    members = jnp.searchsorted(jnp.cumsum(tallies), jnp.arange(rows * top), side="right").astype(jnp.int32)
    table = members.reshape(top, rows).T
    table = table[jax.random.permutation(jax.random.fold_in(own, 1), rows)]
    rotation = jax.random.randint(jax.random.fold_in(own, 2), (rows, 1), 0, top)
    return jnp.take_along_axis(table, (jnp.arange(top)[None, :] + rotation) % top, axis=1)


def load_shares(count, total, bound, skew, full):
    loads = [(1 << 20) // math.isqrt(standing ** skew) + 1 for standing in range(1, count + 1)]
    largest = bound if full else min(bound, max(-(-total // count), total * loads[0] // sum(loads)))
    least = 1 if total - largest >= count - 1 else 0
    holding, spare = [largest] + [least] * (count - 1), total - largest - least * (count - 1)
    while spare > 0:
        free = [i for i in range(1, count) if holding[i] < largest] or [i for i in range(1, count) if holding[i] < bound]
        mass, budget = sum([loads[i] for i in free]), spare
        for i in free:
            more = min(bound - holding[i], max(1, budget * loads[i] // mass), spare)
            holding[i] = holding[i] + more
            spare = spare - more
    return np.array(holding)


def noise(own_key, dims, scale, reach, pieces=(), kind=jnp.bfloat16):
    entries = jax.random.normal(own_key, dims, jnp.float32) * scale
    if len(pieces) > 0:
        entries = steps_of(own_key, dims, pieces, -0.22, 0.18) * entries
    return jnp.clip(entries, min=-reach, max=reach).astype(kind)


def setup_inputs(seed: int = 0) -> dict:
    streams_of = jax.random.split(jax.random.key(seed), 24)
    tokens = noise(streams_of[0], (SEQS, D), 1.0, 6.0, ((0, 4),))
    norm_gain = jnp.clip(1.0 + 0.18 * jax.random.normal(streams_of[1], (D,), jnp.float32), 0.1, 1.9)
    ffn_gain = jnp.clip(1.0 + 0.18 * jax.random.normal(streams_of[2], (D,), jnp.float32), 0.1, 1.9)
    w_in = noise(streams_of[3], (D, GROUPS * CHAN), D ** -0.5, 0.09375, ((1, 8),))
    decay_rate = jnp.clip(jnp.exp(math.log(2.0) - 4.6051702 * jax.random.uniform(streams_of[4], (GROUPS * STATE,), jnp.float32) ** steps_of(streams_of[4], (GROUPS * STATE,), ((0, 8),), -0.2, 0.2)), 0.02, 2.0)
    frequency = jnp.clip(jax.random.uniform(streams_of[5], (GROUPS * STATE,), jnp.float32, -3.140625, 3.140625), -3.140625, 3.140625)
    log_step = jnp.clip(-2.3 + 2.3 * jax.random.uniform(streams_of[6], (GROUPS,), jnp.float32) ** steps_of(streams_of[6], (GROUPS,), ((0, 8),), -0.2, 0.2), -2.3, 0.0)
    input_real = noise(streams_of[7], (CHAN, GROUPS * STATE), (2 * CHAN) ** -0.5, 1.0, ((1, 8),), jnp.float32)
    input_imag = noise(streams_of[8], (CHAN, GROUPS * STATE), (2 * CHAN) ** -0.5, 1.0, ((1, 8),), jnp.float32)
    readout_real = noise(streams_of[9], (CHAN, GROUPS * STATE), (2 * STATE) ** -0.5, 0.5, ((1, 8),), jnp.float32)
    readout_imag = noise(streams_of[10], (CHAN, GROUPS * STATE), (2 * STATE) ** -0.5, 0.5, ((1, 8),), jnp.float32)
    skip_gain = noise(streams_of[11], (GROUPS * CHAN,), 1.0, 4.0, ((0, 8),), jnp.float32)
    state_real = noise(streams_of[12], (SEQS, GROUPS * STATE), 1.0, 6.0, ((0, 4), (1, 8)), jnp.float32)
    state_imag = noise(streams_of[13], (SEQS, GROUPS * STATE), 1.0, 6.0, ((0, 4), (1, 8)), jnp.float32)
    w_out = noise(streams_of[14], (GROUPS * CHAN, D), (GROUPS * CHAN) ** -0.5, 0.125, ((0, 8),))
    shared_gate = noise(streams_of[15], (D, FS), D ** -0.5, 0.09375, ((1, 8),))
    shared_up = noise(streams_of[16], (D, FS), D ** -0.5, 0.09375, ((1, 8),))
    shared_down = noise(streams_of[17], (FS, D), FS ** -0.5, 0.1875, ((0, 8),))
    expert_gate = noise(streams_of[18], (EXPERTS, D, FE), D ** -0.5, 0.09375, ((0, 4), (1, 8)))
    expert_up = noise(streams_of[19], (EXPERTS, D, FE), D ** -0.5, 0.09375, ((0, 4), (1, 8)))
    expert_down = noise(streams_of[20], (EXPERTS, FE, D), FE ** -0.5, 0.1875, ((0, 4), (2, 8)))
    routing_keys = jax.random.split(jax.random.fold_in(streams_of[21], 1), SEQS // SEQ_DEV)
    routing_turns = jax.random.permutation(jax.random.fold_in(streams_of[21], 3), SEQS // SEQ_DEV)
    routing = jax.vmap(lambda own, number: routed_block(jax.random.fold_in(streams_of[21], 2), own, number, SEQ_DEV, EXPERTS, TOP_K, CAP, 2))(routing_keys, routing_turns).reshape((SEQS, TOP_K))
    route_weight = jnp.clip(jnp.exp(math.log(1.0) - 2.3025851 * jax.random.uniform(streams_of[22], (SEQS, TOP_K), jnp.float32) ** steps_of(streams_of[22], (SEQS, TOP_K), ((0, 4),), -0.2, 0.2)), 0.1, 1.0)
    return {"tokens": tokens, "norm_gain": norm_gain, "ffn_gain": ffn_gain, "w_in": w_in, "decay_rate": decay_rate, "frequency": frequency, "log_step": log_step, "input_real": input_real, "input_imag": input_imag, "readout_real": readout_real, "readout_imag": readout_imag, "skip_gain": skip_gain, "state_real": state_real, "state_imag": state_imag, "w_out": w_out, "shared_gate": shared_gate, "shared_up": shared_up, "shared_down": shared_down, "expert_gate": expert_gate, "expert_up": expert_up, "expert_down": expert_down, "routing": routing, "route_weight": route_weight}


EPS = 1e-06
ROUTED_SCALE = 2.5
HIGH = lax.Precision.HIGHEST

def rms_scale(values_in, gains):
    values = values_in.astype(jnp.float32)
    factor = lax.rsqrt(lax.optimization_barrier(jnp.mean(values * values, axis=-1, keepdims=True)) + EPS)
    return (values * factor * gains).astype(jnp.bfloat16)

def state_update(normed, w_in, decay_rate, frequency, log_step, input_real, input_imag, readout_real, readout_imag, skip_gain, state_real, state_imag):
    seq_count = normed.shape[0]
    groups = log_step.shape[0]
    chan_count = skip_gain.shape[0] // groups
    state_width = decay_rate.shape[0] // groups
    drive_rows = jnp.dot(normed, w_in, preferred_element_type=jnp.float32).astype(jnp.bfloat16)
    drive_f = drive_rows.astype(jnp.float32).reshape(seq_count, groups, chan_count)
    decays = decay_rate.reshape(groups, state_width)
    omegas = frequency.reshape(groups, state_width)
    step_size = jnp.exp(log_step)[:, None]
    pole_mag = jnp.exp(-decays * step_size)
    pole_angle = omegas * step_size
    pole_re = pole_mag * jnp.cos(pole_angle)
    pole_im = pole_mag * jnp.sin(pole_angle)
    pole_norm = decays * decays + omegas * omegas
    diff_re = pole_re - 1.0
    lift_re = (-decays * diff_re + omegas * pole_im) / pole_norm
    lift_im = (-decays * pole_im - omegas * diff_re) / pole_norm
    in_re = input_real.reshape(chan_count, groups, state_width)
    in_im = input_imag.reshape(chan_count, groups, state_width)
    push_re = jnp.einsum('sgh,hgp->sgp', drive_f, in_re, precision=HIGH)
    push_im = jnp.einsum('sgh,hgp->sgp', drive_f, in_im, precision=HIGH)
    old_re = state_real.reshape(seq_count, groups, state_width)
    old_im = state_imag.reshape(seq_count, groups, state_width)
    new_re = pole_re * old_re - pole_im * old_im + lift_re * push_re - lift_im * push_im
    new_im = pole_re * old_im + pole_im * old_re + lift_re * push_im + lift_im * push_re
    out_re = readout_real.reshape(chan_count, groups, state_width)
    out_im = readout_imag.reshape(chan_count, groups, state_width)
    read_rows = jnp.einsum('sgp,hgp->sgh', new_re, out_re, precision=HIGH) - jnp.einsum('sgp,hgp->sgh', new_im, out_im, precision=HIGH)
    read_rows = read_rows + skip_gain.reshape(groups, chan_count) * drive_f
    activated = jax.nn.gelu(read_rows).reshape(seq_count, groups * chan_count).astype(jnp.bfloat16)
    return (activated, new_re.reshape(seq_count, groups * state_width), new_im.reshape(seq_count, groups * state_width))

def reference(tokens, norm_gain, ffn_gain, w_in, decay_rate, frequency, log_step, input_real, input_imag, readout_real, readout_imag, skip_gain, state_real, state_imag, w_out, shared_gate, shared_up, shared_down, expert_gate, expert_up, expert_down, routing, route_weight):
    normed = rms_scale(tokens, norm_gain)
    activated, new_real, new_imag = state_update(normed, w_in, decay_rate, frequency, log_step, input_real, input_imag, readout_real, readout_imag, skip_gain, state_real, state_imag)
    mixer_terms = jnp.dot(activated, w_out, preferred_element_type=jnp.float32)
    resid = (tokens.astype(jnp.float32) + mixer_terms).astype(jnp.bfloat16)
    ffn_rows = rms_scale(resid, ffn_gain)
    shared_gate_rows = jnp.dot(ffn_rows, shared_gate, preferred_element_type=jnp.float32)
    shared_up_rows = jnp.dot(ffn_rows, shared_up, preferred_element_type=jnp.float32)
    shared_inner = (jax.nn.silu(shared_gate_rows) * shared_up_rows).astype(jnp.bfloat16)
    shared = jnp.dot(shared_inner, shared_down, preferred_element_type=jnp.float32)
    seq_total = tokens.shape[0]
    expert_count = expert_gate.shape[0]
    block_count = seq_total // SEQ_DEV
    per_block = SEQ_DEV * TOP_K
    flat_ids = routing.reshape(-1).astype(jnp.int32)
    one_hot = (flat_ids[:, None] == jnp.arange(expert_count, dtype=jnp.int32)[None, :]).astype(jnp.int32)
    blocked = one_hot.reshape(block_count, per_block, expert_count)
    earlier = (jnp.cumsum(blocked, axis=1) - blocked).reshape(seq_total * TOP_K, expert_count)
    slot_rank = lax.optimization_barrier(jnp.sum(earlier * one_hot, axis=1)).astype(jnp.int32)
    block_ids = (jnp.arange(seq_total * TOP_K, dtype=jnp.int32) // per_block).astype(jnp.int32)
    buffer_rows = block_count * CAP
    column = (block_ids * CAP + slot_rank).astype(jnp.int32)
    token_ids = (jnp.arange(seq_total * TOP_K, dtype=jnp.int32) // TOP_K).astype(jnp.int32)
    table = jnp.full((expert_count, buffer_rows), seq_total, jnp.int32).at[flat_ids, column].set(token_ids)
    padded = jnp.concatenate([ffn_rows, jnp.zeros((1, ffn_rows.shape[1]), jnp.bfloat16)], axis=0)

    def one_expert(args):
        index_rows, gate_w, up_w, down_w = args
        picked = padded[index_rows].astype(jnp.float32)
        gate_rows = jnp.dot(picked, gate_w.astype(jnp.float32), preferred_element_type=jnp.float32)
        up_rows = jnp.dot(picked, up_w.astype(jnp.float32), preferred_element_type=jnp.float32)
        inner_rows = (jax.nn.silu(gate_rows) * up_rows).astype(jnp.bfloat16)
        return jnp.dot(inner_rows.astype(jnp.float32), down_w.astype(jnp.float32), preferred_element_type=jnp.float32)
    outputs = lax.map(one_expert, (table, expert_gate, expert_up, expert_down))
    flat_out = outputs.reshape(expert_count * buffer_rows, outputs.shape[2])
    picked_rows = flat_out[(flat_ids * buffer_rows + column).astype(jnp.int32)].reshape(seq_total, TOP_K, outputs.shape[2])
    weights = route_weight / lax.optimization_barrier(jnp.sum(route_weight, axis=1, keepdims=True)) * ROUTED_SCALE
    routed = lax.optimization_barrier(jnp.sum(weights[:, :, None] * picked_rows, axis=1))
    mixed = (resid.astype(jnp.float32) + shared + routed).astype(jnp.bfloat16)
    return (mixed, new_real, new_imag)
```

```python
import functools

import jax
import jax.numpy as jnp
from jax import lax
from jax.experimental import pallas as pl
from jax.experimental.pallas import tpu as pltpu
from jax.sharding import PartitionSpec as P


EPS = 1e-06
ROUTED_SCALE = 2.5
LANES = 128
MIB = 1 << 20
HIGH = lax.Precision.HIGHEST
F32 = jnp.float32
BF16 = jnp.bfloat16
IN_VMEM = pl.BlockSpec(memory_space=pltpu.VMEM)
IN_SMEM = pl.BlockSpec(memory_space=pltpu.SMEM)
IN_HBM = pl.BlockSpec(memory_space=pltpu.HBM)


def in_hbm(*arrays):
    return [pltpu.with_memory_space_constraint(x, pltpu.HBM) for x in arrays]


def dot(a, b, **kwargs):
    return jnp.dot(a, b, preferred_element_type=F32, **kwargs)


def partner(index, step, size):
    return index ^ step if size & (size - 1) == 0 else (index + step) % size


def back(index, step, size):
    return index ^ step if size & (size - 1) == 0 else (index - step) % size


def tp_layout():
    size = lax.axis_size("tp")
    return size // 2, [(i, i ^ 1) for i in range(size)]


def send_line(blocks):
    chips = tp_layout()[0]
    got = [blocks[0]]
    for step in range(1, chips):
        pairs = [
            (2 * z + c, 2 * partner(z, step, chips) + c) for z in range(chips) for c in range(2)
        ]
        got.append(lax.ppermute(blocks[step], "tp", pairs))
    return got


def send_ep(blocks):
    size = lax.axis_size("ep")
    got = [blocks[0]]
    for step in range(1, size):
        pairs = [(i, partner(i, step, size)) for i in range(size)]
        got.append(lax.ppermute(blocks[step], "ep", pairs))
    return got


def pair_sum(keep, give):
    chips, swap = tp_layout()
    got = lax.ppermute(give, "tp", swap)
    return [(keep[j] + got[j].astype(F32)).astype(BF16) for j in range(chips)]


def line_gather(block):
    chips, swap = tp_layout()
    mine = send_line([block] * chips)
    return mine, [lax.ppermute(b, "tp", swap) for b in mine]


def total_of(blocks):
    out = blocks[0].astype(F32)
    for block in blocks[1:]:
        out = out + block.astype(F32)
    return out


def call(kernel, out_shape, in_specs, scratch=(), limit=24):
    specs = jax.tree.map(lambda leaf: IN_VMEM, out_shape)
    return pl.pallas_call(
        kernel,
        out_shape=out_shape,
        in_specs=in_specs,
        out_specs=specs,
        scratch_shapes=list(scratch),
        compiler_params=pltpu.CompilerParams(vmem_limit_bytes=limit * MIB),
    )


def column_block(ref, index, width):
    return ref[:, pl.ds(pl.multiple_of(index * width, width), width)]


def load_all(sources, targets, sems):
    copies = [
        pltpu.make_async_copy(a, b, sems.at[i]) for i, (a, b) in enumerate(zip(sources, targets))
    ]
    for copy in copies:
        copy.start()
    return copies


def state_kernel(chips, spot_ref, log_step, *refs):
    sources, (keep, give, new_re, new_im) = refs[:13], refs[13:17]
    targets, acts, sems = refs[17:30], refs[30], refs[31]
    (
        tokens, gain, w_in, decay, omega, in_re, in_im, old_re, old_im, read_re, read_im, skip, w_out
    ) = targets
    copies = load_all(sources, targets, sems)
    copies[0].wait()
    copies[1].wait()
    groups = log_step.shape[0]
    chan_count = in_re.shape[0]
    channels, states = skip.shape[1], decay.shape[1]
    width = states // groups
    values = tokens[...].astype(F32)
    factor = lax.rsqrt(jnp.mean(values * values, axis=1, keepdims=True) + EPS)
    normed = (values * factor * gain[...]).astype(BF16)

    group_of = lax.broadcasted_iota(jnp.int32, (1, states), 1) // width
    step = jnp.zeros((1, states), F32)
    for g in range(groups):
        step = jnp.where(group_of == g, log_step[g], step)
    step = jnp.exp(step)
    copies[3].wait()
    copies[4].wait()
    decays, omegas = decay[...], omega[...]
    size = jnp.exp(-decays * step)
    angle = omegas * step
    pole_re, pole_im = size * jnp.cos(angle), size * jnp.sin(angle)
    norm = decays * decays + omegas * omegas
    diff = pole_re - 1.0
    lift_re = (-decays * diff + omegas * pole_im) / norm
    lift_im = (-decays * pole_im - omegas * diff) / norm

    copies[2].wait()
    for copy in copies[5:12]:
        copy.wait()
    drive = dot(normed, w_in[...]).astype(BF16).astype(F32)
    block = min(channels, LANES)
    span = block // chan_count * width
    row = lax.broadcasted_iota(jnp.int32, (block, span), 0) // chan_count
    col = lax.broadcasted_iota(jnp.int32, (block, span), 1) // width
    same = row == col

    def spread(ref, at):
        part = ref[:, at : at + span]
        return jnp.where(same, jnp.concatenate([part] * (block // chan_count), axis=0), 0.0)

    for b in range(channels // block):
        at = b * span
        here = slice(at, at + span)
        part = drive[:, b * block : (b + 1) * block]
        push_re = dot(part, spread(in_re, at), precision=HIGH)
        push_im = dot(part, spread(in_im, at), precision=HIGH)
        was_re, was_im = old_re[:, here], old_im[:, here]
        p_re, p_im, l_re, l_im = pole_re[:, here], pole_im[:, here], lift_re[:, here], lift_im[:, here]
        now_re = p_re * was_re - p_im * was_im + l_re * push_re - l_im * push_im
        now_im = p_re * was_im + p_im * was_re + l_re * push_im + l_im * push_re
        new_re[:, here] = now_re
        new_im[:, here] = now_im
        across = (((1,), (1,)), ((), ()))
        read = lax.dot_general(
            now_re, spread(read_re, at), across, precision=HIGH, preferred_element_type=F32
        ) - lax.dot_general(
            now_im, spread(read_im, at), across, precision=HIGH, preferred_element_type=F32
        )
        read = read + skip[:, b * block : (b + 1) * block] * part
        acts[:, b * block : (b + 1) * block] = jax.nn.gelu(read).astype(BF16)
    copies[12].wait()
    emit_columns(chips, spot_ref, acts[...], w_out, keep, give)


def emit_columns(chips, spot_ref, rows, weights, keep, give):
    side, chip = spot_ref[0], spot_ref[2]
    slice_width = keep.shape[2]
    for j in range(chips):
        to = 2 * partner(chip, j, chips)
        keep[j] = dot(rows, column_block(weights, to + side, slice_width))
        give[j] = dot(rows, column_block(weights, to + 1 - side, slice_width)).astype(BF16)


def shared_kernel(chips, spot_ref, gain, *refs):
    side, chip = spot_ref[0], spot_ref[2]
    mine, other, sources = refs[:chips], refs[chips : 2 * chips], refs[2 * chips : 2 * chips + 3]
    keep, give = refs[2 * chips + 3 : 2 * chips + 5]
    gate, up, down, sems = refs[2 * chips + 5 :]
    copies = load_all(sources, (gate, up, down), sems)
    seq_count, slice_width = mine[0].shape
    total = jnp.zeros((seq_count, 1), F32)
    for part in mine + other:
        values = part[...].astype(F32)
        total = total + jnp.sum(values * values, axis=1, keepdims=True)
    factor = lax.rsqrt(total / (2 * chips * slice_width) + EPS)
    gate_rows = jnp.zeros((seq_count, gate.shape[1]), F32)
    up_rows = gate_rows
    copies[0].wait()
    copies[1].wait()
    for j in range(chips):
        source = 2 * back(chip, j, chips)
        for part, index in ((mine[j], source + side), (other[j], source + 1 - side)):
            scaled = part[...].astype(F32) * factor * column_block(gain, index, slice_width)
            rows = scaled.astype(BF16)
            here = pl.ds(pl.multiple_of(index * slice_width, slice_width), slice_width)
            gate_rows = gate_rows + dot(rows, gate[here, :])
            up_rows = up_rows + dot(rows, up[here, :])
    inner = (jax.nn.silu(gate_rows) * up_rows).astype(BF16)
    copies[2].wait()
    emit_columns(chips, spot_ref, inner, down, keep, give)


def placement(spot_ref, code, expert_dev, expert_count):
    first = spot_ref[1]
    token_count, lanes = code.shape
    row = lax.broadcasted_iota(jnp.int32, (8, lanes), 0)
    col = lax.broadcasted_iota(jnp.int32, (8, lanes), 1)
    pick = (row < expert_dev) & ((col == first + row) | (col == first + row + expert_count))
    across = (((1,), (1,)), ((), ()))
    weights = lax.dot_general(
        pick.astype(F32).astype(BF16), code, across, preferred_element_type=F32
    )
    taken = (weights > 0).astype(F32)
    square = (token_count, token_count)
    earlier = lax.broadcasted_iota(jnp.int32, square, 0) < lax.broadcasted_iota(jnp.int32, square, 1)
    before = dot(taken.astype(BF16), earlier.astype(F32).astype(BF16))
    loads = jnp.sum(taken, axis=1, keepdims=True)
    starts, so_far = [], jnp.zeros((1, 1), F32)
    for e in range(expert_dev):
        starts.append(so_far)
        so_far = so_far + loads[e : e + 1]
    starts.append(so_far)
    return weights, taken, before, starts


def expert_kernel(chips, ep_count, expert_count, spot_ref, gain, *refs):
    parts, (gate_hbm, up_hbm) = refs[:ep_count], refs[ep_count : ep_count + 2]
    keep, give, gate, up, message, scaled, acc, sems = refs[ep_count + 2 :]
    expert_dev, slice_width, hidden = gate.shape
    copies = [
        load_all((gate_hbm.at[e], up_hbm.at[e]), (gate.at[e], up.at[e]), sems.at[e])
        for e in range(expert_dev)
    ]
    side, chip = spot_ref[0], spot_ref[2]
    slots = acc.shape[0]
    share = slots // (2 * chips)
    rows = parts[0].shape[0]
    for j in range(ep_count):
        message[j * rows : (j + 1) * rows] = parts[j][...]
    token_count = message.shape[0]
    code = message[:, slice_width:]
    _, taken, before, starts = placement(spot_ref, code, expert_dev, expert_count)
    slot = lax.broadcasted_iota(jnp.int32, (slots, token_count), 0).astype(F32)
    hit = jnp.zeros((slots, token_count), F32)
    for e in range(expert_dev):
        place = jnp.where(taken[e : e + 1] > 0, before[e : e + 1] + starts[e], -1.0)
        hit = hit + (slot == place).astype(F32)
    picked = dot(hit.astype(BF16), message[:, :slice_width])
    squares = picked * picked
    lanes = squares[:, :LANES]
    for at in range(LANES, slice_width, LANES):
        lanes = lanes + squares[:, at : at + LANES]
    scaled[...] = (picked * gain[...]).astype(BF16)
    acc[:, : 2 * hidden] = jnp.zeros((slots, 2 * hidden), F32)
    acc[:, 2 * hidden :] = lanes
    bounds = [jnp.max(s).astype(jnp.int32) for s in starts]
    tile = min(slots, LANES)
    for e in range(expert_dev):
        for copy in copies[e]:
            copy.wait()
        for t in range(0, slots, tile):
            size = min(tile, slots - t)
            here = lax.broadcasted_iota(jnp.int32, (size, 1), 0) + t

            @pl.when((bounds[e] < t + size) & (bounds[e + 1] > t))
            def _():
                inside = (here >= bounds[e]) & (here < bounds[e + 1])
                rows = jnp.where(inside, scaled[t : t + size].astype(F32), 0.0).astype(BF16)
                acc[t : t + size, :hidden] += dot(rows, gate[e])
                acc[t : t + size, hidden : 2 * hidden] += dot(rows, up[e])
    for j in range(chips):
        to = 2 * partner(chip, j, chips)
        keep[j] = acc[pl.ds(pl.multiple_of((to + side) * share, 8), share), :]
        at = pl.multiple_of((to + 1 - side) * share, 8)
        give[j] = acc[pl.ds(at, share), :].astype(BF16)


def inner_kernel(model_width, *refs):
    sums, out = refs[:-1], refs[-1]
    hidden = out.shape[1]
    total = total_of([part[...] for part in sums])
    square = jnp.sum(total[:, 2 * hidden :], axis=1, keepdims=True)
    factor = lax.rsqrt(square / model_width + EPS)
    gate, up = total[:, :hidden] * factor, total[:, hidden : 2 * hidden] * factor
    out[...] = (jax.nn.silu(gate) * up).astype(BF16)


def down_kernel(chips, ep_count, expert_count, spot_ref, *refs):
    mine, other, refs = refs[:chips], refs[chips : 2 * chips], refs[2 * chips :]
    parts, down_hbm, outs = refs[:ep_count], refs[ep_count], refs[ep_count + 1 : 2 * ep_count + 1]
    down, code, wide, acc, sems = refs[2 * ep_count + 1 :]
    expert_dev, _, slice_width = down.shape
    copies = load_all(
        [down_hbm.at[e] for e in range(expert_dev)], [down.at[e] for e in range(expert_dev)], sems
    )
    side, chip = spot_ref[0], spot_ref[2]
    slots = acc.shape[0]
    share = mine[0].shape[0]
    rows = parts[0].shape[0]
    for j in range(ep_count):
        code[j * rows : (j + 1) * rows] = parts[j][:, slice_width:]
    token_count = code.shape[0]
    weights, taken, before, starts = placement(spot_ref, code[...], expert_dev, expert_count)
    for j in range(chips):
        source = 2 * back(chip, j, chips)
        for part, index in ((mine[j], source + side), (other[j], source + 1 - side)):
            wide[pl.ds(pl.multiple_of(index * share, 8), share), :] = part[...].astype(F32)
    bounds = [jnp.max(s).astype(jnp.int32) for s in starts]
    acc[...] = jnp.zeros(acc.shape, F32)
    tile = min(slots, LANES)
    for e in range(expert_dev):
        copies[e].wait()
        for t in range(0, slots, tile):
            size = min(tile, slots - t)
            here = lax.broadcasted_iota(jnp.int32, (size, 1), 0) + t

            @pl.when((bounds[e] < t + size) & (bounds[e + 1] > t))
            def _():
                inside = (here >= bounds[e]) & (here < bounds[e + 1])
                rows = jnp.where(inside, wide[t : t + size], 0.0).astype(BF16)
                acc[t : t + size, :] += dot(rows, down[e])
    slot = lax.broadcasted_iota(jnp.int32, (slots, token_count), 0).astype(F32)
    mix = jnp.zeros((slots, token_count), F32)
    for e in range(expert_dev):
        place = jnp.where(taken[e : e + 1] > 0, before[e : e + 1] + starts[e], -1.0)
        mix = mix + jnp.where(slot == place, weights[e : e + 1], 0.0)
    total = lax.dot_general(
        mix.astype(BF16),
        acc[...].astype(BF16),
        (((0,), (0,)), ((), ())),
        preferred_element_type=F32,
    )
    for j in range(ep_count):
        outs[j][...] = total[j * rows : (j + 1) * rows].astype(BF16)


def routed_experts(slots, spot, message, gain_own, model_width, expert_gate, expert_up, expert_down):
    chips, _ = tp_layout()
    ep_count = lax.axis_size("ep")
    expert_dev, slice_width, hidden = expert_gate.shape
    expert_count = expert_dev * ep_count
    seq_count, message_width = message[0].shape
    token_count = seq_count * ep_count
    share = slots // (2 * chips)
    columns = 2 * hidden + LANES
    keep, give = call(
        functools.partial(expert_kernel, chips, ep_count, expert_count),
        (
            jax.ShapeDtypeStruct((chips, share, columns), F32),
            jax.ShapeDtypeStruct((chips, share, columns), BF16),
        ),
        [IN_SMEM] + [IN_VMEM] * (1 + ep_count) + [IN_HBM] * 2,
        (
            pltpu.VMEM(expert_gate.shape, BF16),
            pltpu.VMEM(expert_up.shape, BF16),
            pltpu.VMEM((token_count, message_width), BF16),
            pltpu.VMEM((slots, slice_width), BF16),
            pltpu.VMEM((slots, columns), F32),
            pltpu.SemaphoreType.DMA((expert_dev, 2)),
        ),
    )(spot, gain_own, *message, *in_hbm(expert_gate, expert_up))
    sums = send_line(pair_sum(keep, give))
    inner = call(
        functools.partial(inner_kernel, model_width),
        jax.ShapeDtypeStruct((share, hidden), BF16),
        [IN_VMEM] * chips,
    )(*sums)
    mine, other = line_gather(inner)
    return call(
        functools.partial(down_kernel, chips, ep_count, expert_count),
        [jax.ShapeDtypeStruct((seq_count, slice_width), BF16)] * ep_count,
        [IN_SMEM] + [IN_VMEM] * (2 * chips + ep_count) + [IN_HBM],
        (
            pltpu.VMEM(expert_down.shape, BF16),
            pltpu.VMEM((token_count, message_width - slice_width), BF16),
            pltpu.VMEM((slots, hidden), F32),
            pltpu.VMEM((slots, slice_width), F32),
            pltpu.SemaphoreType.DMA((expert_dev,)),
        ),
    )(spot, *mine, *other, *message, *in_hbm(expert_down))


def local(
    tokens,
    norm_gain,
    ffn_gain,
    w_in,
    decay_rate,
    frequency,
    log_step,
    input_real,
    input_imag,
    readout_real,
    readout_imag,
    skip_gain,
    state_real,
    state_imag,
    w_out,
    shared_gate,
    shared_up,
    shared_down,
    expert_gate,
    expert_up,
    expert_down,
    routing,
    route_weight,
):
    seq_count, model_width = tokens.shape
    chips, _ = tp_layout()
    ep_count = lax.axis_size("ep")
    slice_width = model_width // (2 * chips)
    expert_dev = expert_gate.shape[0]
    expert_count = expert_dev * ep_count
    me = lax.axis_index("tp")
    offset = me * slice_width
    first = lax.axis_index("ep") * expert_dev
    at = jnp.arange(3)
    spot = jnp.where(at == 0, me % 2, jnp.where(at == 1, first, me // 2)).astype(jnp.int32)
    columns = (
        jax.ShapeDtypeStruct((chips, seq_count, slice_width), F32),
        jax.ShapeDtypeStruct((chips, seq_count, slice_width), BF16),
    )
    operands = (
        tokens,
        norm_gain[None],
        w_in,
        decay_rate[None],
        frequency[None],
        input_real,
        input_imag,
        state_real,
        state_imag,
        readout_real,
        readout_imag,
        skip_gain[None],
        w_out,
    )
    keep, give, new_real, new_imag = call(
        functools.partial(state_kernel, chips),
        columns
        + (
            jax.ShapeDtypeStruct(state_real.shape, F32),
            jax.ShapeDtypeStruct(state_imag.shape, F32),
        ),
        [IN_SMEM, IN_SMEM] + [IN_HBM] * len(operands),
        [pltpu.VMEM(x.shape, x.dtype) for x in operands]
        + [
            pltpu.VMEM((seq_count, w_out.shape[0]), BF16),
            pltpu.SemaphoreType.DMA((len(operands),)),
        ],
    )(spot, log_step, *in_hbm(*operands))
    arrived = send_line(pair_sum(keep, give))
    own_tokens = lax.dynamic_slice_in_dim(tokens, offset, slice_width, 1).astype(F32)
    resid_own = (own_tokens + total_of(arrived)).astype(BF16)
    gain_own = lax.dynamic_slice_in_dim(ffn_gain, offset, slice_width, 0)[None]

    top_count = routing.shape[1]
    weights = route_weight / jnp.sum(route_weight, axis=1, keepdims=True) * ROUTED_SCALE
    named = routing[:, :, None] == jnp.arange(expert_count, dtype=jnp.int32)
    dense = jnp.sum(jnp.where(named, weights[:, :, None], 0.0), axis=1)
    high = lax.reduce_precision(dense, 8, 7)
    code = jnp.concatenate([high, dense - high], axis=1)
    code = jnp.pad(code, ((0, 0), (0, -code.shape[1] % LANES))).astype(BF16)
    message = jnp.concatenate([resid_own, code], axis=1)
    message = send_ep([message] * ep_count)
    capacity = 2 * seq_count * top_count // expert_count
    slots = expert_dev * ep_count * capacity

    resid_mine, resid_other = line_gather(resid_own)
    combined = routed_experts(
        slots, spot, message, gain_own, model_width, expert_gate, expert_up, expert_down
    )
    keep, give = call(
        functools.partial(shared_kernel, chips),
        columns,
        [IN_SMEM] + [IN_VMEM] * (1 + 2 * chips) + [IN_HBM] * 3,
        [pltpu.VMEM(x.shape, BF16) for x in (shared_gate, shared_up, shared_down)]
        + [pltpu.SemaphoreType.DMA((3,))],
    )(
        spot,
        ffn_gain[None],
        *resid_mine,
        *resid_other,
        *in_hbm(shared_gate, shared_up, shared_down),
    )
    shared = send_line(pair_sum(keep, give))
    returned = send_ep(combined)
    mixed = (resid_own.astype(F32) + total_of(shared) + total_of(returned)).astype(BF16)
    return (mixed, new_real, new_imag)


def solution(mesh):
    placed = (
        P("ep", None),
        P(),
        P(),
        P(None, "tp"),
        P("tp"),
        P("tp"),
        P("tp"),
        P(None, "tp"),
        P(None, "tp"),
        P(None, "tp"),
        P(None, "tp"),
        P("tp"),
        P("ep", "tp"),
        P("ep", "tp"),
        P("tp", None),
        P(None, "tp"),
        P(None, "tp"),
        P("tp", None),
        P("ep", "tp", None),
        P("ep", "tp", None),
        P("ep", None, "tp"),
        P("ep", None),
        P("ep", None),
    )
    return jax.shard_map(
        local,
        mesh=mesh,
        in_specs=placed,
        out_specs=(P("ep", "tp"), P("ep", "tp"), P("ep", "tp")),
        check_vma=False,
    )
```

```python
import functools

import jax
import jax.numpy as jnp
from jax import lax
from jax.experimental import pallas as pl
from jax.experimental.pallas import tpu as pltpu
from jax.sharding import PartitionSpec as P


EPS = 1e-06
ROUTED_SCALE = 2.5
LANES = 128
ROWS = 16
MIB = 1 << 20
HIGH = lax.Precision.HIGHEST
F32 = jnp.float32
BF16 = jnp.bfloat16
IN_VMEM = pl.BlockSpec(memory_space=pltpu.VMEM)
IN_SMEM = pl.BlockSpec(memory_space=pltpu.SMEM)
IN_HBM = pl.BlockSpec(memory_space=pltpu.HBM)


def in_hbm(*arrays):
    return [pltpu.with_memory_space_constraint(x, pltpu.HBM) for x in arrays]


def dot(a, b, **kwargs):
    return jnp.dot(a, b, preferred_element_type=F32, **kwargs)


def partner(index, step, size):
    return index ^ step if size & (size - 1) == 0 else (index + step) % size


def back(index, step, size):
    return index ^ step if size & (size - 1) == 0 else (index - step) % size


def tp_layout():
    size = lax.axis_size("tp")
    return size // 2, [(i, i ^ 1) for i in range(size)]


def send_line(blocks):
    chips = tp_layout()[0]
    got = [blocks[0]]
    for step in range(1, chips):
        pairs = [
            (2 * z + c, 2 * partner(z, step, chips) + c) for z in range(chips) for c in range(2)
        ]
        got.append(lax.ppermute(blocks[step], "tp", pairs))
    return got


def send_ep(blocks):
    size = lax.axis_size("ep")
    got = [blocks[0]]
    for step in range(1, size):
        pairs = [(i, partner(i, step, size)) for i in range(size)]
        got.append(lax.ppermute(blocks[step], "ep", pairs))
    return got


def pair_sum(keep, give):
    chips, swap = tp_layout()
    got = lax.ppermute(give, "tp", swap)
    return [(keep[j] + got[j].astype(F32)).astype(BF16) for j in range(chips)]


def line_gather(block):
    chips, swap = tp_layout()
    mine = send_line([block] * chips)
    return mine, [lax.ppermute(b, "tp", swap) for b in mine]


def total_of(blocks):
    out = blocks[0].astype(F32)
    for block in blocks[1:]:
        out = out + block.astype(F32)
    return out


def call(kernel, out_shape, in_specs, scratch=(), limit=24):
    specs = jax.tree.map(lambda leaf: IN_VMEM, out_shape)
    return pl.pallas_call(
        kernel,
        out_shape=out_shape,
        in_specs=in_specs,
        out_specs=specs,
        scratch_shapes=list(scratch),
        compiler_params=pltpu.CompilerParams(vmem_limit_bytes=limit * MIB),
    )


def column_block(ref, index, width):
    return ref[:, pl.ds(pl.multiple_of(index * width, width), width)]


def load_all(sources, targets, sems):
    copies = [
        pltpu.make_async_copy(a, b, sems.at[i]) for i, (a, b) in enumerate(zip(sources, targets))
    ]
    for copy in copies:
        copy.start()
    return copies


def preload_kernel(*refs):
    count = len(refs) // 2
    for copy in load_all(refs[:count], refs[count:-1], refs[-1]):
        copy.wait()


def preload(*arrays):
    return pl.pallas_call(
        preload_kernel,
        out_shape=[pltpu.VMEM(x.shape, x.dtype) for x in arrays],
        in_specs=[IN_HBM] * len(arrays),
        out_specs=[IN_VMEM] * len(arrays),
        scratch_shapes=[pltpu.SemaphoreType.DMA((len(arrays),))],
        compiler_params=pltpu.CompilerParams(vmem_limit_bytes=MIB),
    )(*in_hbm(*arrays))


def state_kernel(chips, spot_ref, *refs):
    sources, (keep, give, new_re, new_im) = refs[:14], refs[14:18]
    targets, acts, sems = refs[18:32], refs[32], refs[33]
    (
        tokens, gain, w_in, decay, omega, in_re, in_im, old_re, old_im, read_re, read_im, skip, w_out, log_step
    ) = targets
    copies = load_all(sources, targets, sems)
    copies[0].wait()
    copies[1].wait()
    groups = log_step.shape[0]
    chan_count = in_re.shape[0]
    channels, states = skip.shape[1], decay.shape[1]
    width = states // groups
    values = tokens[...].astype(F32)
    factor = lax.rsqrt(jnp.mean(values * values, axis=1, keepdims=True) + EPS)
    normed = (values * factor * gain[...]).astype(BF16)

    group_of = lax.broadcasted_iota(jnp.int32, (1, states), 1) // width
    step = jnp.zeros((1, states), F32)
    copies[13].wait()
    for g in range(groups):
        step = jnp.where(group_of == g, log_step[g], step)
    step = jnp.exp(step)
    copies[3].wait()
    copies[4].wait()
    decays, omegas = decay[...], omega[...]
    size = jnp.exp(-decays * step)
    angle = omegas * step
    pole_re, pole_im = size * jnp.cos(angle), size * jnp.sin(angle)
    norm = decays * decays + omegas * omegas
    diff = pole_re - 1.0
    lift_re = (-decays * diff + omegas * pole_im) / norm
    lift_im = (-decays * pole_im - omegas * diff) / norm

    copies[2].wait()
    for copy in copies[5:12]:
        copy.wait()
    drive = dot(normed, w_in[...]).astype(BF16).astype(F32)
    block = min(channels, LANES)
    span = block // chan_count * width
    row = lax.broadcasted_iota(jnp.int32, (block, span), 0) // chan_count
    col = lax.broadcasted_iota(jnp.int32, (block, span), 1) // width
    same = row == col

    def spread(ref, at):
        part = ref[:, at : at + span]
        return jnp.where(same, jnp.concatenate([part] * (block // chan_count), axis=0), 0.0)

    for b in range(channels // block):
        at = b * span
        here = slice(at, at + span)
        part = drive[:, b * block : (b + 1) * block]
        push_re = dot(part, spread(in_re, at), precision=HIGH)
        push_im = dot(part, spread(in_im, at), precision=HIGH)
        was_re, was_im = old_re[:, here], old_im[:, here]
        p_re, p_im, l_re, l_im = pole_re[:, here], pole_im[:, here], lift_re[:, here], lift_im[:, here]
        now_re = p_re * was_re - p_im * was_im + l_re * push_re - l_im * push_im
        now_im = p_re * was_im + p_im * was_re + l_re * push_im + l_im * push_re
        new_re[:, here] = now_re
        new_im[:, here] = now_im
        across = (((1,), (1,)), ((), ()))
        read = lax.dot_general(
            now_re, spread(read_re, at), across, precision=HIGH, preferred_element_type=F32
        ) - lax.dot_general(
            now_im, spread(read_im, at), across, precision=HIGH, preferred_element_type=F32
        )
        read = read + skip[:, b * block : (b + 1) * block] * part
        acts[:, b * block : (b + 1) * block] = jax.nn.gelu(read).astype(BF16)
    copies[12].wait()
    emit_columns(chips, spot_ref, acts[...], w_out, keep, give)


def emit_columns(chips, spot_ref, rows, weights, keep, give):
    side, chip = spot_ref[0], spot_ref[2]
    slice_width = keep.shape[2]
    for j in range(chips):
        to = 2 * partner(chip, j, chips)
        keep[j] = dot(rows, column_block(weights, to + side, slice_width))
        give[j] = dot(rows, column_block(weights, to + 1 - side, slice_width)).astype(BF16)


def shared_kernel(chips, spot_ref, gain, *refs):
    side, chip = spot_ref[0], spot_ref[2]
    mine, other, sources = refs[:chips], refs[chips : 2 * chips], refs[2 * chips : 2 * chips + 3]
    keep, give = refs[2 * chips + 3 : 2 * chips + 5]
    gate, up, down, sems = refs[2 * chips + 5 :]
    copies = load_all(sources, (gate, up, down), sems)
    seq_count, slice_width = mine[0].shape
    total = jnp.zeros((seq_count, 1), F32)
    for part in mine + other:
        values = part[...].astype(F32)
        total = total + jnp.sum(values * values, axis=1, keepdims=True)
    factor = lax.rsqrt(total / (2 * chips * slice_width) + EPS)
    gate_rows = jnp.zeros((seq_count, gate.shape[1]), F32)
    up_rows = gate_rows
    copies[0].wait()
    copies[1].wait()
    for j in range(chips):
        source = 2 * back(chip, j, chips)
        for part, index in ((mine[j], source + side), (other[j], source + 1 - side)):
            scaled = part[...].astype(F32) * factor * column_block(gain, index, slice_width)
            rows = scaled.astype(BF16)
            here = pl.ds(pl.multiple_of(index * slice_width, slice_width), slice_width)
            gate_rows = gate_rows + dot(rows, gate[here, :])
            up_rows = up_rows + dot(rows, up[here, :])
    inner = (jax.nn.silu(gate_rows) * up_rows).astype(BF16)
    copies[2].wait()
    emit_columns(chips, spot_ref, inner, down, keep, give)


def placement(spot_ref, code, expert_dev, expert_count):
    first = spot_ref[1]
    token_count, lanes = code.shape
    row = lax.broadcasted_iota(jnp.int32, (8, lanes), 0)
    col = lax.broadcasted_iota(jnp.int32, (8, lanes), 1)
    pick = (row < expert_dev) & ((col == first + row) | (col == first + row + expert_count))
    across = (((1,), (1,)), ((), ()))
    weights = lax.dot_general(
        pick.astype(F32).astype(BF16), code, across, preferred_element_type=F32
    )
    taken = (weights > 0).astype(F32)
    square = (token_count, token_count)
    earlier = lax.broadcasted_iota(jnp.int32, square, 0) < lax.broadcasted_iota(jnp.int32, square, 1)
    before = dot(taken.astype(BF16), earlier.astype(F32).astype(BF16))
    loads = jnp.sum(taken, axis=1, keepdims=True)
    starts, so_far = [], jnp.zeros((1, 1), F32)
    for e in range(expert_dev):
        starts.append(so_far)
        so_far = so_far + loads[e : e + 1]
    starts.append(so_far)
    return weights, taken, before, starts


def expert_window(bounds, e, expert_dev, slots):
    size = slots // expert_dev + ROWS
    first = bounds[e] // ROWS * ROWS
    row = lax.broadcasted_iota(jnp.int32, (size, 1), 0) + first
    inside = (row >= bounds[e]) & (row < bounds[e + 1])
    return pl.ds(pl.multiple_of(first, ROWS), size), inside


def expert_kernel(chips, ep_count, expert_count, spot_ref, gain, *refs):
    parts, (gate, up) = refs[:ep_count], refs[ep_count : ep_count + 2]
    emitted, (over, message, scaled, acc) = refs[ep_count + 2 : -4], refs[-4:]
    expert_dev, slice_width, hidden = gate.shape
    side, chip = spot_ref[0], spot_ref[2]
    slots = acc.shape[0] - ROWS
    rows = parts[0].shape[0]
    for j in range(ep_count):
        message[j * rows : (j + 1) * rows] = parts[j][...]
    token_count = message.shape[0]
    code = message[:, slice_width:]
    _, taken, before, starts = placement(spot_ref, code, expert_dev, expert_count)
    named = jnp.sum((code > 0).astype(F32), axis=0, keepdims=True)
    group = lax.broadcasted_iota(jnp.int32, named.shape, 1) // expert_dev
    most = jnp.zeros((1, 1), F32)
    for g in range(ep_count):
        load = jnp.sum(jnp.where(group == g, named, 0.0), axis=1, keepdims=True)
        most = jnp.maximum(most, load)
    over[0] = (jnp.max(most) > 2 * chips * emitted[0].shape[1]).astype(jnp.int32)
    slot = lax.broadcasted_iota(jnp.int32, (slots, token_count), 0).astype(F32)
    hit = jnp.zeros((slots, token_count), F32)
    for e in range(expert_dev):
        place = jnp.where(taken[e : e + 1] > 0, before[e : e + 1] + starts[e], -1.0)
        hit = hit + (slot == place).astype(F32)
    picked = dot(hit.astype(BF16), message[:, :slice_width])
    squares = picked * picked
    lanes = squares[:, :LANES]
    for at in range(LANES, slice_width, LANES):
        lanes = lanes + squares[:, at : at + LANES]
    scaled[:slots] = (picked * gain[...]).astype(BF16)
    acc[:slots, 2 * hidden :] = lanes
    bounds = [jnp.max(s).astype(jnp.int32) for s in starts]
    for t in range(0, slots, LANES):
        size = min(LANES, slots - t)

        @pl.when(bounds[-1] < t + size)
        def _():
            acc[t : t + size, : 2 * hidden] = jnp.zeros((size, 2 * hidden), F32)

    for e in range(expert_dev):
        window, inside = expert_window(bounds, e, expert_dev, slots)
        rows = scaled[window, :]
        for at, weight in ((0, gate), (hidden, up)):
            part = dot(rows, weight[e])
            acc[window, at : at + hidden] = jnp.where(inside, part, acc[window, at : at + hidden])

    base = 0
    for keep, give in zip(emitted[::2], emitted[1::2]):
        share = keep.shape[1]
        for j in range(chips):
            to = 2 * partner(chip, j, chips)
            at = pl.multiple_of(base + (to + side) * share, 8)
            keep[j] = acc[pl.ds(at, share), :]
            at = pl.multiple_of(base + (to + 1 - side) * share, 8)
            give[j] = acc[pl.ds(at, share), :].astype(BF16)
        base += 2 * chips * share


def inner_kernel(model_width, *refs):
    sums, out = refs[:-1], refs[-1]
    hidden = out.shape[1]
    total = total_of([part[...] for part in sums])
    square = jnp.sum(total[:, 2 * hidden :], axis=1, keepdims=True)
    factor = lax.rsqrt(square / model_width + EPS)
    gate, up = total[:, :hidden] * factor, total[:, hidden : 2 * hidden] * factor
    out[...] = (jax.nn.silu(gate) * up).astype(BF16)


def down_kernel(chips, ep_count, expert_count, spot_ref, *refs):
    mine, other, refs = refs[:chips], refs[chips : 2 * chips], refs[2 * chips :]
    parts, down, refs = refs[:ep_count], refs[ep_count], refs[ep_count + 1 :]
    rest, outs, (code, wide, acc) = refs[: -ep_count - 3], refs[-ep_count - 3 : -3], refs[-3:]
    expert_dev, _, slice_width = down.shape
    side, chip = spot_ref[0], spot_ref[2]
    slots = acc.shape[0] - ROWS
    share = mine[0].shape[0]
    rows = parts[0].shape[0]
    for j in range(ep_count):
        code[j * rows : (j + 1) * rows] = parts[j][:, slice_width:]
    token_count = code.shape[0]
    weights, taken, before, starts = placement(spot_ref, code[...], expert_dev, expert_count)
    for j in range(chips):
        source = 2 * back(chip, j, chips)
        for part, index in ((mine[j], source + side), (other[j], source + 1 - side)):
            wide[pl.ds(pl.multiple_of(index * share, 8), share), :] = part[...]
            for more in rest:
                extra = more.shape[1]
                at = 2 * chips * share + index * extra
                block = more[j if part is mine[j] else chips + j]
                wide[pl.ds(pl.multiple_of(at, 8), extra), :] = block
    bounds = [jnp.max(s).astype(jnp.int32) for s in starts]
    acc[...] = jnp.zeros(acc.shape, F32)
    for e in range(expert_dev):
        window, inside = expert_window(bounds, e, expert_dev, slots)
        part = dot(wide[window, :], down[e])
        acc[window, :] = jnp.where(inside, part, acc[window, :])
    slot = lax.broadcasted_iota(jnp.int32, (slots, token_count), 0).astype(F32)
    mix = jnp.zeros((slots, token_count), F32)
    for e in range(expert_dev):
        place = jnp.where(taken[e : e + 1] > 0, before[e : e + 1] + starts[e], -1.0)
        mix = mix + jnp.where(slot == place, weights[e : e + 1], 0.0)
    total = lax.dot_general(
        mix.astype(BF16),
        acc[:slots].astype(BF16),
        (((0,), (0,)), ((), ())),
        preferred_element_type=F32,
    )
    for j in range(ep_count):
        outs[j][...] = total[j * rows : (j + 1) * rows].astype(BF16)


def routed_experts(slots, spot, message, gain_own, model_width, gate_up, expert_down):
    chips, _ = tp_layout()
    ep_count = lax.axis_size("ep")
    expert_dev, slice_width, hidden = gate_up[0].shape
    expert_count = expert_dev * ep_count
    seq_count, message_width = message[0].shape
    token_count = seq_count * ep_count
    columns = 2 * hidden + LANES
    tail = slots // 4
    step = 16 * chips
    shares = [slots // (2 * chips)]
    if tail % step == 0 and (slots - tail) % step == 0:
        shares = [(slots - tail) // (2 * chips), tail // (2 * chips)]
    emitted = [
        jax.ShapeDtypeStruct((chips, share, columns), kind) for share in shares for kind in (F32, BF16)
    ]
    *emitted, over = pl.pallas_call(
        functools.partial(expert_kernel, chips, ep_count, expert_count),
        name="expert_in",
        out_shape=emitted + [jax.ShapeDtypeStruct((1,), jnp.int32)],
        in_specs=[IN_SMEM] + [IN_VMEM] * (3 + ep_count),
        out_specs=[IN_VMEM] * len(emitted) + [IN_SMEM],
        scratch_shapes=[
            pltpu.VMEM((token_count, message_width), BF16),
            pltpu.VMEM((slots + ROWS, slice_width), BF16),
            pltpu.VMEM((slots + ROWS, columns), F32),
        ],
        compiler_params=pltpu.CompilerParams(vmem_limit_bytes=20 * MIB),
    )(spot, gain_own, *message, *gate_up)

    def through(keep, give):
        sums = send_line(pair_sum(keep, give))
        inner = call(
            functools.partial(inner_kernel, model_width),
            jax.ShapeDtypeStruct((keep.shape[1], hidden), BF16),
            [IN_VMEM] * chips,
        )(*sums)
        return line_gather(inner)

    def more(keep, give):
        mine, other = through(keep, give)
        return jnp.stack(mine + other)

    def none(keep, give):
        return jnp.zeros((2 * chips, keep.shape[1], hidden), BF16)

    mine, other = through(*emitted[:2])
    rest = []
    if len(shares) > 1:
        rest = [lax.cond(over[0] > 0, more, none, *emitted[2:])]
        rest[0], expert_down = lax.optimization_barrier((rest[0], expert_down))
    (down,) = preload(expert_down)
    return call(
        functools.partial(down_kernel, chips, ep_count, expert_count),
        [jax.ShapeDtypeStruct((seq_count, slice_width), BF16)] * ep_count,
        [IN_SMEM] + [IN_VMEM] * (2 * chips + ep_count + 1 + len(rest)),
        (
            pltpu.VMEM((token_count, message_width - slice_width), BF16),
            pltpu.VMEM((slots + ROWS, hidden), BF16),
            pltpu.VMEM((slots + ROWS, slice_width), F32),
        ),
        limit=16,
    )(spot, *mine, *other, *message, down, *rest)


def local(
    tokens,
    norm_gain,
    ffn_gain,
    w_in,
    decay_rate,
    frequency,
    log_step,
    input_real,
    input_imag,
    readout_real,
    readout_imag,
    skip_gain,
    state_real,
    state_imag,
    w_out,
    shared_gate,
    shared_up,
    shared_down,
    expert_gate,
    expert_up,
    expert_down,
    routing,
    route_weight,
):
    seq_count, model_width = tokens.shape
    chips, _ = tp_layout()
    ep_count = lax.axis_size("ep")
    slice_width = model_width // (2 * chips)
    expert_dev = expert_gate.shape[0]
    expert_count = expert_dev * ep_count
    me = lax.axis_index("tp")
    offset = me * slice_width
    first = lax.axis_index("ep") * expert_dev
    at = jnp.arange(3)
    spot = jnp.where(at == 0, me % 2, jnp.where(at == 1, first, me // 2)).astype(jnp.int32)
    columns = (
        jax.ShapeDtypeStruct((chips, seq_count, slice_width), F32),
        jax.ShapeDtypeStruct((chips, seq_count, slice_width), BF16),
    )
    operands = (
        tokens,
        norm_gain[None],
        w_in,
        decay_rate[None],
        frequency[None],
        input_real,
        input_imag,
        state_real,
        state_imag,
        readout_real,
        readout_imag,
        skip_gain[None],
        w_out,
        log_step,
    )
    keep, give, new_real, new_imag = call(
        functools.partial(state_kernel, chips),
        columns
        + (
            jax.ShapeDtypeStruct(state_real.shape, F32),
            jax.ShapeDtypeStruct(state_imag.shape, F32),
        ),
        [IN_SMEM] + [IN_HBM] * len(operands),
        [pltpu.VMEM(x.shape, x.dtype) for x in operands[:-1]]
        + [
            pltpu.SMEM(log_step.shape, F32),
            pltpu.VMEM((seq_count, w_out.shape[0]), BF16),
            pltpu.SemaphoreType.DMA((len(operands),)),
        ],
    )(spot, *in_hbm(*operands))
    arrived = send_line(pair_sum(keep, give))
    gate_up = preload(expert_gate, expert_up)
    own_tokens = lax.dynamic_slice_in_dim(tokens, offset, slice_width, 1).astype(F32)
    resid_own = (own_tokens + total_of(arrived)).astype(BF16)
    gain_own = lax.dynamic_slice_in_dim(ffn_gain, offset, slice_width, 0)[None]

    top_count = routing.shape[1]
    weights = route_weight / jnp.sum(route_weight, axis=1, keepdims=True) * ROUTED_SCALE
    named = routing[:, :, None] == jnp.arange(expert_count, dtype=jnp.int32)
    dense = jnp.sum(jnp.where(named, weights[:, :, None], 0.0), axis=1)
    high = lax.reduce_precision(dense, 8, 7)
    code = jnp.concatenate([high, dense - high], axis=1)
    code = jnp.pad(code, ((0, 0), (0, -code.shape[1] % LANES))).astype(BF16)
    message = jnp.concatenate([resid_own, code], axis=1)
    message = send_ep([message] * ep_count)
    capacity = 2 * seq_count * top_count // expert_count
    slots = expert_dev * ep_count * capacity

    resid_mine, resid_other = line_gather(resid_own)
    combined = routed_experts(
        slots, spot, message, gain_own, model_width, gate_up, expert_down
    )
    keep, give = call(
        functools.partial(shared_kernel, chips),
        columns,
        [IN_SMEM] + [IN_VMEM] * (1 + 2 * chips) + [IN_HBM] * 3,
        [pltpu.VMEM(x.shape, BF16) for x in (shared_gate, shared_up, shared_down)]
        + [pltpu.SemaphoreType.DMA((3,))],
    )(
        spot,
        ffn_gain[None],
        *resid_mine,
        *resid_other,
        *in_hbm(shared_gate, shared_up, shared_down),
    )
    shared = pair_sum(keep, give)
    shared = send_line(shared)
    returned = send_ep(combined)
    mixed = (resid_own.astype(F32) + total_of(shared) + total_of(returned)).astype(BF16)
    return (mixed, new_real, new_imag)


def solution(mesh):
    placed = (
        P("ep", None),
        P(),
        P(),
        P(None, "tp"),
        P("tp"),
        P("tp"),
        P("tp"),
        P(None, "tp"),
        P(None, "tp"),
        P(None, "tp"),
        P(None, "tp"),
        P("tp"),
        P("ep", "tp"),
        P("ep", "tp"),
        P("tp", None),
        P(None, "tp"),
        P(None, "tp"),
        P("tp", None),
        P("ep", "tp", None),
        P("ep", "tp", None),
        P("ep", None, "tp"),
        P("ep", None),
        P("ep", None),
    )
    return jax.shard_map(
        local,
        mesh=mesh,
        in_specs=placed,
        out_specs=(P("ep", "tp"), P("ep", "tp"), P("ep", "tp")),
        check_vma=False,
    )
```
